32 devices in a mesh: sp: 4 (over y, x), dp: 8 (over z, core).
Axes of the slice: x: 2, y: 2, z: 4, core: 2. Of those that a mesh axis runs over, the one named last changes fastest.
Arguments:
- tokens: bfloat16 [8, 1536, 2048], P('dp', 'sp'), may hold values from -6 to 6
- value_act: bfloat16 [8, 1536, 1024], P('dp', 'sp'), may hold values from -6 to 6
- gate_act: bfloat16 [8, 1536, 1024], P('dp', 'sp'), may hold values from -6 to 6
- cotangent: bfloat16 [8, 1536, 1024], P('dp', 'sp'), may hold values from -6 to 6
- value_weight: bfloat16 [2048, 1024], P('dp'), may hold values from -0.1875 to 0.1875
- gate_weight: bfloat16 [2048, 1024], P('dp'), may hold values from -0.1875 to 0.1875
- norm_gain: float32 [1024], replicated, may hold values from 0.1 to 1.9
- norm_bias: float32 [1024], replicated, may hold values from -3 to 3
- mix_weight: bfloat16 [16, 128, 128], replicated, may hold values from -0.5 to 0.5
- mix_bias: float32 [16, 128], replicated, may hold values from 0.1 to 1.9
Outputs:
- tokens_grad: bfloat16 [8, 1536, 2048], P('dp', 'sp')
- value_weight_grad: float32 [2048, 1024], P('dp')
- gate_weight_grad: float32 [2048, 1024], P('dp')
- mix_weight_grad: float32 [16, 128, 128], replicated
- mix_bias_grad: float32 [16, 128], replicated
- norm_gain_grad: float32 [1024], replicated
- norm_bias_grad: float32 [1024], replicated
The draws below stay inside these ranges and needn't reach their ends.
All inputs are finite; a program needn't handle non-finite values.
Results may differ from the reference program's by a relative error of at most 0.0054.
Values may be sent and summed in bfloat16 or wider, within the bound.
No kernel may reach another device: no remote copies, remote signals or barrier semaphores. Data moves between devices by JAX's collectives and lax.ppermute only.
A program may use at most 128 MiB of HBM per device.

```python
import jax
import jax.numpy as jnp
from jax import lax

D = 2048
GROUPS = 16
DG = 1024
BLOCK = 128
SEQ = 1536
SEQS = 8


def strengthened(array, stream_key, source, target, parts, factor):
    owner, partner = [(jnp.arange(array.shape[dim]) // (array.shape[dim] // parts)).reshape([-1 if axis == dim else 1 for axis in range(array.ndim)]) for dim in (source, target)]
    chosen = jax.random.permutation(stream_key, parts)[partner]
    strong = (owner == chosen) | (owner == (partner + parts // 2) % parts)
    return jnp.where(strong, factor * array, array)


def block_scale(rng, shape, split, least, high):
    level, own = 1.0, jax.random.fold_in(rng, 6)
    for axis_at, parts in split:
        steps = jnp.exp(jax.random.uniform(jax.random.fold_in(own, axis_at), (parts,), jnp.float32, least / len(split), high / len(split)))
        level = level * jnp.repeat(steps, shape[axis_at] // parts).reshape([-1 if axis == axis_at else 1 for axis in range(len(shape))])
    return level


def scatter_about(stream_key, dims, scale, bound, split=(), kind=jnp.bfloat16):
    loudness = block_scale(stream_key, dims, split, -0.22, 0.18) if split else 1.0
    values = jax.random.normal(stream_key, dims, jnp.float32) * scale * loudness
    return jnp.minimum(jnp.maximum(values, -bound), bound).astype(kind)


def noise_with(stream_key, dims, spread, most, shards, heavy, kind=jnp.bfloat16):
    array = spread * jax.random.normal(stream_key, dims, jnp.float32)
    if shards:
        array = array * block_scale(stream_key, dims, shards, -0.22, 0.18)
    return jnp.clip(strengthened(array, jax.random.fold_in(stream_key, 3), *heavy), -most, most).astype(kind)


def setup_inputs(seed: int = 0) -> dict:
    key_of = jax.random.split(jax.random.key(seed), 11)
    tokens = noise_with(key_of[0], (SEQS, SEQ, D), 1.0, 6.0, ((0, 8), (1, 4)), (1, 2, 4, 2.0))
    value_act = scatter_about(key_of[1], (SEQS, SEQ, DG), 1.0, 6.0, ((0, 8), (1, 4)))
    gate_act = scatter_about(key_of[2], (SEQS, SEQ, DG), 1.0, 6.0, ((0, 8), (1, 4)))
    cotangent = scatter_about(key_of[3], (SEQS, SEQ, DG), 1.0, 6.0, ((0, 8), (1, 4)))
    value_weight = scatter_about(key_of[4], (D, DG), DG ** -0.5, 0.1875, ((0, 8),))
    gate_weight = scatter_about(key_of[5], (D, DG), DG ** -0.5, 0.1875, ((0, 8),))
    norm_gain = jnp.clip(1.0 + 0.18 * jax.random.normal(key_of[6], (DG,), jnp.float32), 0.1, 1.9)
    norm_bias = scatter_about(key_of[7], (DG,), 0.5, 3.0, (), jnp.float32)
    mix_weight = scatter_about(key_of[8], (GROUPS, BLOCK, BLOCK), BLOCK ** -0.5, 0.5)
    mix_bias = jnp.clip(1.0 + 0.18 * jax.random.normal(key_of[9], (GROUPS, BLOCK), jnp.float32), 0.1, 1.9)
    return {"tokens": tokens, "value_act": value_act, "gate_act": gate_act, "cotangent": cotangent, "value_weight": value_weight, "gate_weight": gate_weight, "norm_gain": norm_gain, "norm_bias": norm_bias, "mix_weight": mix_weight, "mix_bias": mix_bias}


EPSILON = 1e-06

def gelu_slope(values):
    cdf_part = 0.5 * (1.0 + lax.erf(values * 0.7071067811865476))
    pdf_part = jnp.exp(-0.5 * values * values) * 0.3989422804014327
    return cdf_part + values * pdf_part

def mixer_backward(value_act, gate_act, cotangent, norm_gain, norm_bias, mix_weight, mix_bias):
    seq_len, channels = value_act.shape
    groups, block_len = (mix_weight.shape[0], mix_weight.shape[1])
    group_dim = channels // groups
    blocks = seq_len // block_len
    value_float = value_act.astype(jnp.float32)
    gate_float = gate_act.astype(jnp.float32)
    activated = jax.nn.gelu(value_float, approximate=False)
    gate_gelu = jax.nn.gelu(gate_float, approximate=False)
    centred = gate_gelu - lax.optimization_barrier(jnp.mean(gate_gelu, axis=-1, keepdims=True))
    inv_std = lax.rsqrt(lax.optimization_barrier(jnp.mean(centred * centred, axis=-1, keepdims=True)) + EPSILON)
    normed = centred * inv_std
    spread_in = (normed * norm_gain + norm_bias).astype(jnp.bfloat16)
    spread_in = spread_in.reshape(blocks, block_len, groups, group_dim)
    causal = jnp.tril(jnp.ones((block_len, block_len), dtype=bool))
    masked_weight = jnp.where(causal[None], mix_weight, jnp.zeros_like(mix_weight))
    spatial = jnp.einsum('gts,bsgd->btgd', masked_weight.astype(jnp.float32), spread_in.astype(jnp.float32))
    spatial = (spatial + mix_bias.T[None, :, :, None]).reshape(seq_len, channels)
    grad_out = cotangent.astype(jnp.float32)
    grad_act = grad_out * spatial
    grad_spatial = grad_out * activated
    grad_split = grad_spatial.reshape(blocks, block_len, groups, group_dim)
    bias_grad = lax.optimization_barrier(jnp.sum(grad_split, axis=(0, 3))).T
    spatial_low = grad_split.astype(jnp.bfloat16)
    weight_grad = jnp.einsum('btgd,bsgd->gts', spatial_low.astype(jnp.float32), spread_in.astype(jnp.float32))
    weight_grad = jnp.where(causal[None], weight_grad, jnp.zeros_like(weight_grad))
    grad_norm = jnp.einsum('gts,btgd->bsgd', masked_weight.astype(jnp.float32), spatial_low.astype(jnp.float32))
    grad_norm = grad_norm.reshape(seq_len, channels)
    gain_grad = lax.optimization_barrier(jnp.sum(grad_norm * normed, axis=0))
    shift_grad = lax.optimization_barrier(jnp.sum(grad_norm, axis=0))
    grad_hat = grad_norm * norm_gain
    grad_gate = inv_std * (grad_hat - lax.optimization_barrier(jnp.mean(grad_hat, axis=-1, keepdims=True)) - normed * lax.optimization_barrier(jnp.mean(grad_hat * normed, axis=-1, keepdims=True)))
    value_grad = (grad_act * gelu_slope(value_float)).astype(jnp.bfloat16)
    gate_grad = (grad_gate * gelu_slope(gate_float)).astype(jnp.bfloat16)
    return (value_grad, gate_grad, (weight_grad, bias_grad, gain_grad, shift_grad))

def reference(tokens, value_act, gate_act, cotangent, value_weight, gate_weight, norm_gain, norm_bias, mix_weight, mix_bias):
    both_weights = jnp.concatenate((value_weight, gate_weight), axis=1)

    def per_sequence(running, seq_items):
        inputs, value_seq, gate_seq, cot_seq = seq_items
        value_grad, gate_grad, stats = mixer_backward(value_seq, gate_seq, cot_seq, norm_gain, norm_bias, mix_weight, mix_bias)
        both_grads = jnp.concatenate((value_grad, gate_grad), axis=1)
        input_grad = jnp.dot(both_grads, both_weights.T, preferred_element_type=jnp.float32).astype(jnp.bfloat16)
        weight_sums = running[0] + jnp.dot(inputs.T, both_grads, preferred_element_type=jnp.float32)
        updated = (weight_sums,) + tuple((old + term for old, term in zip(running[1:], stats)))
        return (updated, input_grad)
    initial = (jnp.zeros((D, 2 * DG), jnp.float32), jnp.zeros((GROUPS, BLOCK, BLOCK), jnp.float32), jnp.zeros((GROUPS, BLOCK), jnp.float32), jnp.zeros((DG,), jnp.float32), jnp.zeros((DG,), jnp.float32))
    running, input_grads = lax.scan(per_sequence, initial, (tokens, value_act, gate_act, cotangent))
    return (input_grads, running[0][:, :DG], running[0][:, DG:], running[1], running[2], running[3], running[4])
```

```python
import jax
import jax.numpy as jnp
from jax import lax
from jax.sharding import PartitionSpec as P

EPSILON = 1e-06


def gelu_slope(values):
    cdf_part = 0.5 * (1.0 + lax.erf(values * 0.7071067811865476))
    pdf_part = jnp.exp(-0.5 * values * values) * 0.3989422804014327
    return cdf_part + values * pdf_part


def mixer_backward(value_act, gate_act, cotangent, norm_gain, norm_bias, mix_weight, mix_bias):
    seq_len, channels = value_act.shape
    groups, block_len = (mix_weight.shape[0], mix_weight.shape[1])
    group_dim = channels // groups
    blocks = seq_len // block_len
    value_float = value_act.astype(jnp.float32)
    gate_float = gate_act.astype(jnp.float32)
    activated = jax.nn.gelu(value_float, approximate=False)
    gate_gelu = jax.nn.gelu(gate_float, approximate=False)
    centred = gate_gelu - jnp.mean(gate_gelu, axis=-1, keepdims=True)
    inv_std = lax.rsqrt(jnp.mean(centred * centred, axis=-1, keepdims=True) + EPSILON)
    normed = centred * inv_std
    spread_in = (normed * norm_gain + norm_bias).astype(jnp.bfloat16)
    spread_in = spread_in.reshape(blocks, block_len, groups, group_dim)
    causal = jnp.tril(jnp.ones((block_len, block_len), dtype=bool))
    masked_weight = jnp.where(causal[None], mix_weight, jnp.zeros_like(mix_weight))
    spatial = jnp.einsum(
        "gts,bsgd->btgd", masked_weight, spread_in, preferred_element_type=jnp.float32
    )
    spatial = (spatial + mix_bias.T[None, :, :, None]).reshape(seq_len, channels)
    grad_out = cotangent.astype(jnp.float32)
    grad_act = grad_out * spatial
    grad_spatial = grad_out * activated
    grad_split = grad_spatial.reshape(blocks, block_len, groups, group_dim)
    bias_grad = jnp.sum(grad_split, axis=(0, 3)).T
    spatial_low = grad_split.astype(jnp.bfloat16)
    weight_grad = jnp.einsum(
        "btgd,bsgd->gts", spatial_low, spread_in, preferred_element_type=jnp.float32
    )
    weight_grad = jnp.where(causal[None], weight_grad, jnp.zeros_like(weight_grad))
    grad_norm = jnp.einsum(
        "gts,btgd->bsgd", masked_weight, spatial_low, preferred_element_type=jnp.float32
    )
    grad_norm = grad_norm.reshape(seq_len, channels)
    gain_grad = jnp.sum(grad_norm * normed, axis=0)
    shift_grad = jnp.sum(grad_norm, axis=0)
    grad_hat = grad_norm * norm_gain
    grad_gate = inv_std * (
        grad_hat
        - jnp.mean(grad_hat, axis=-1, keepdims=True)
        - normed * jnp.mean(grad_hat * normed, axis=-1, keepdims=True)
    )
    value_grad = (grad_act * gelu_slope(value_float)).astype(jnp.bfloat16)
    gate_grad = (grad_gate * gelu_slope(gate_float)).astype(jnp.bfloat16)
    return (value_grad, gate_grad, (weight_grad, bias_grad, gain_grad, shift_grad))


CORES = 2


def swap(array, axis, mask):
    ways = lax.axis_size(axis)
    return lax.ppermute(array, axis, [(here, here ^ mask) for here in range(ways)])


def pick(array, index):
    return lax.dynamic_index_in_dim(array, index, 0, keepdims=False)


def exchange_add(pieces, here, axis, ways, stride):
    arrived = [
        swap(pick(pieces, here ^ step).astype(jnp.bfloat16), axis, step * stride)
        for step in range(1, ways)
    ]
    total = pick(pieces, here)
    for term in arrived:
        total = total + term.astype(jnp.float32)
    return total


def weight_rows(lhs, grads, seq_here, core, depth):
    seq_ways = lax.axis_size("sp")
    depth_ways = lax.axis_size("dp") // CORES
    dims = (((1,), (0,)), ((), ()))
    away = lax.dot_general(
        pick(lhs, 1 - core), grads, dims, preferred_element_type=jnp.float32
    ).astype(jnp.bfloat16)
    arrived = swap(away, "dp", 1)
    own = lax.dot_general(pick(lhs, core), grads, dims, preferred_element_type=jnp.float32)
    own = own + arrived.astype(jnp.float32)
    rows, channels = own.shape
    own = own.reshape(seq_ways, rows // seq_ways, channels)
    own = exchange_add(own, seq_here, "sp", seq_ways, 1)
    own = own.reshape(depth_ways, -1, channels)
    own = exchange_add(own, depth, "dp", depth_ways, CORES).astype(jnp.bfloat16)
    parts = [own] + [swap(own, "sp", step) for step in range(1, seq_ways)]
    stacked = jnp.stack(parts)
    return jnp.concatenate(
        [pick(stacked, seq_here ^ place) for place in range(seq_ways)], axis=0
    ).astype(jnp.float32)


def sum_everywhere(wide, small):
    for axis in ("dp", "sp"):
        mask = 1
        while mask < lax.axis_size(axis):
            kept = lax.reduce_precision(wide, 8, 7)
            wide = kept + swap(kept.astype(jnp.bfloat16), axis, mask).astype(jnp.float32)
            small = small + swap(small, axis, mask)
            mask *= 2
    return wide, small


def shards(
    tokens,
    value_act,
    gate_act,
    cotangent,
    value_weight,
    gate_weight,
    norm_gain,
    norm_bias,
    mix_weight,
    mix_bias,
):
    seq_ways = lax.axis_size("sp")
    data_ways = lax.axis_size("dp")
    seq_here = lax.axis_index("sp")
    data_here = lax.axis_index("dp")
    core = data_here % CORES
    depth = data_here // CORES
    inputs = tokens[0]
    seq_len, width = inputs.shape
    part_rows = width // (seq_ways * data_ways)
    lhs = (
        inputs.reshape(seq_len, data_ways // CORES, CORES, seq_ways, part_rows)
        .transpose(2, 3, 1, 4, 0)
        .reshape(CORES, width // CORES, seq_len)
    )
    both_weights = lax.all_gather(
        jnp.concatenate((value_weight, gate_weight), axis=1), "dp", axis=0, tiled=True
    )
    value_grad, gate_grad, stats = mixer_backward(
        value_act[0], gate_act[0], cotangent[0], norm_gain, norm_bias, mix_weight, mix_bias
    )
    value_rows = weight_rows(lhs, value_grad, seq_here, core, depth)
    gate_rows = weight_rows(lhs, gate_grad, seq_here, core, depth)
    groups, block_len = mix_bias.shape
    lanes = stats[1].shape[1]
    packed = jnp.concatenate(
        (stats[1], stats[2].reshape(-1, lanes), stats[3].reshape(-1, lanes)), axis=0
    )
    wide, small = sum_everywhere(stats[0], packed)
    gain_end = groups + stats[2].size // lanes
    input_grad = lax.dot_general(
        jnp.concatenate((value_grad, gate_grad), axis=1),
        both_weights,
        (((1,), (1,)), ((), ())),
        preferred_element_type=jnp.float32,
    ).astype(jnp.bfloat16)
    return (
        input_grad[None],
        value_rows,
        gate_rows,
        wide,
        small[:groups],
        small[groups:gain_end].reshape(-1),
        small[gain_end:].reshape(-1),
    )


def solution(mesh):
    placed = (
        P("dp", "sp", None),
        P("dp", "sp", None),
        P("dp", "sp", None),
        P("dp", "sp", None),
        P("dp", None),
        P("dp", None),
        P(),
        P(),
        P(),
        P(),
    )
    return jax.shard_map(
        shards,
        mesh=mesh,
        in_specs=placed,
        out_specs=(P("dp", "sp", None), P("dp", None), P("dp", None), P(), P(), P(), P()),
        check_vma=False,
    )
```

```python
import jax
import jax.numpy as jnp
from jax import lax
from jax.sharding import PartitionSpec as P

EPSILON = 1e-06


def gelu_slope(values):
    cdf_part = 0.5 * (1.0 + lax.erf(values * 0.7071067811865476))
    pdf_part = jnp.exp(-0.5 * values * values) * 0.3989422804014327
    return cdf_part + values * pdf_part


def mixer_backward(value_act, gate_act, cotangent, norm_gain, norm_bias, mix_weight, mix_bias):
    seq_len, channels = value_act.shape
    groups, block_len = (mix_weight.shape[0], mix_weight.shape[1])
    group_dim = channels // groups
    blocks = seq_len // block_len
    value_float = value_act.astype(jnp.float32)
    gate_float = gate_act.astype(jnp.float32)
    activated = jax.nn.gelu(value_float, approximate=False)
    gate_gelu = jax.nn.gelu(gate_float, approximate=False)
    centred = gate_gelu - jnp.mean(gate_gelu, axis=-1, keepdims=True)
    inv_std = lax.rsqrt(jnp.mean(centred * centred, axis=-1, keepdims=True) + EPSILON)
    normed = centred * inv_std
    spread_in = (normed * norm_gain + norm_bias).astype(jnp.bfloat16)
    spread_in = spread_in.reshape(blocks, block_len, groups, group_dim)
    causal = jnp.tril(jnp.ones((block_len, block_len), dtype=bool))
    masked_weight = jnp.where(causal[None], mix_weight, jnp.zeros_like(mix_weight))
    spatial = jnp.einsum(
        "gts,bsgd->btgd", masked_weight, spread_in, preferred_element_type=jnp.float32
    )
    spatial = (spatial + mix_bias.T[None, :, :, None]).reshape(seq_len, channels)
    grad_out = cotangent.astype(jnp.float32)
    grad_act = grad_out * spatial
    grad_spatial = grad_out * activated
    grad_split = grad_spatial.reshape(blocks, block_len, groups, group_dim)
    bias_grad = jnp.sum(grad_split, axis=(0, 3)).T
    spatial_low = grad_split.astype(jnp.bfloat16)
    weight_grad = jnp.einsum(
        "btgd,bsgd->gts", spatial_low, spread_in, preferred_element_type=jnp.float32
    )
    weight_grad = jnp.where(causal[None], weight_grad, jnp.zeros_like(weight_grad))
    grad_norm = jnp.einsum(
        "gts,btgd->bsgd", masked_weight, spatial_low, preferred_element_type=jnp.float32
    )
    grad_norm = grad_norm.reshape(seq_len, channels)
    gain_grad = jnp.sum(grad_norm * normed, axis=0)
    shift_grad = jnp.sum(grad_norm, axis=0)
    grad_hat = grad_norm * norm_gain
    grad_gate = inv_std * (
        grad_hat
        - jnp.mean(grad_hat, axis=-1, keepdims=True)
        - normed * jnp.mean(grad_hat * normed, axis=-1, keepdims=True)
    )
    value_grad = (grad_act * gelu_slope(value_float)).astype(jnp.bfloat16)
    gate_grad = (grad_gate * gelu_slope(gate_float)).astype(jnp.bfloat16)
    return (value_grad, gate_grad, (weight_grad, bias_grad, gain_grad, shift_grad))


CORES = 2


def swap(array, axis, mask):
    ways = lax.axis_size(axis)
    return lax.ppermute(array, axis, [(here, here ^ mask) for here in range(ways)])


def pick(array, index):
    return lax.dynamic_index_in_dim(array, index, 0, keepdims=False)


def joined(main, extra):
    main = main.astype(jnp.bfloat16)
    if extra is None:
        return main
    return jnp.concatenate((main, extra.astype(jnp.bfloat16)), axis=-2)


def added(main, extra, arrived):
    rows = main.shape[-2]
    arrived = arrived.astype(jnp.float32)
    main = main + arrived[..., :rows, :]
    return main, None if extra is None else extra + arrived[..., rows:, :]


def picked(main, extra, index):
    return pick(main, index), None if extra is None else pick(extra, index)


def exchange_add(main, extra, here, axis, ways, stride):
    arrived = [
        swap(joined(*picked(main, extra, here ^ step)), axis, step * stride)
        for step in range(1, ways)
    ]
    main, extra = picked(main, extra, here)
    for term in arrived:
        main, extra = added(main, extra, term)
    return main, extra


def gathered(own, here, axis, ways, stride):
    parts = [own] + [swap(own, axis, step * stride) for step in range(1, ways)]
    stacked = jnp.stack(parts)
    return jnp.stack([pick(stacked, here ^ place) for place in range(ways)])


def first_sums(lhs, grads, extra, seq_here, core):
    seq_ways = lax.axis_size("sp")
    depth_ways = lax.axis_size("dp") // CORES
    dims = (((1,), (0,)), ((), ()))

    def terms(index):
        product = lax.dot_general(
            pick(lhs, index), grads, dims, preferred_element_type=jnp.float32
        )
        return product.reshape(seq_ways, depth_ways, -1, product.shape[1])

    away_extra = None if extra is None else pick(extra, 1 - core)
    arrived = swap(joined(terms(1 - core), away_extra), "dp", 1)
    main, extra = added(terms(core), None if extra is None else pick(extra, core), arrived)
    return exchange_add(main, extra, seq_here, "sp", seq_ways, 1)


def last_sums(main, extra, seq_here, depth):
    depth_ways = lax.axis_size("dp") // CORES
    main, extra = exchange_add(main, extra, depth, "dp", depth_ways, CORES)
    rows = main.shape[0]
    pieces = gathered(joined(main, extra), seq_here, "sp", lax.axis_size("sp"), 1)
    return pieces[:, :rows].reshape(-1, pieces.shape[2]).astype(jnp.float32), pieces[:, rows:]


def shards(
    tokens,
    value_act,
    gate_act,
    cotangent,
    value_weight,
    gate_weight,
    norm_gain,
    norm_bias,
    mix_weight,
    mix_bias,
):
    seq_ways = lax.axis_size("sp")
    data_ways = lax.axis_size("dp")
    seq_here = lax.axis_index("sp")
    data_here = lax.axis_index("dp")
    core = data_here % CORES
    depth = data_here // CORES
    inputs = tokens[0]
    seq_len, width = inputs.shape
    part_rows = width // (seq_ways * data_ways)
    lhs = (
        inputs.reshape(seq_len, data_ways // CORES, CORES, seq_ways, part_rows)
        .transpose(2, 3, 1, 4, 0)
        .reshape(CORES, width // CORES, seq_len)
    )
    both_weights = lax.all_gather(
        jnp.concatenate((value_weight, gate_weight), axis=1), "dp", axis=0, tiled=True
    )
    value_grad, gate_grad, stats = mixer_backward(
        value_act[0], gate_act[0], cotangent[0], norm_gain, norm_bias, mix_weight, mix_bias
    )
    channels = value_grad.shape[1]
    depth_ways = data_ways // CORES
    places = (CORES, seq_ways, depth_ways)
    pieces = seq_ways * data_ways
    small = jnp.concatenate([term.reshape(-1) for term in stats[1:]])
    small_part = small.size // pieces
    wide_rows = stats[0].size // (pieces * channels)
    extra = jnp.concatenate(
        (
            stats[0].reshape(places + (wide_rows, channels)),
            jnp.pad(
                small.reshape(places + (1, small_part)),
                ((0, 0),) * 4 + ((0, channels - small_part),),
            ),
        ),
        axis=-2,
    )
    value_sums = first_sums(lhs, value_grad, extra, seq_here, core)
    gate_sums = first_sums(lhs, gate_grad, None, seq_here, core)
    input_grad = lax.dot_general(
        jnp.concatenate((value_grad, gate_grad), axis=1),
        both_weights,
        (((1,), (1,)), ((), ())),
        preferred_element_type=jnp.float32,
    ).astype(jnp.bfloat16)
    value_rows, totals = last_sums(*value_sums, seq_here, depth)
    gate_main, input_grad = lax.optimization_barrier((gate_sums[0], input_grad))
    gate_rows, _ = last_sums(gate_main, None, seq_here, depth)
    totals = gathered(totals, depth, "dp", depth_ways, CORES)
    totals = gathered(totals, core, "dp", CORES, 1)
    totals = totals.transpose(0, 2, 1, 3, 4).astype(jnp.float32)
    wide = totals[..., :wide_rows, :].reshape(stats[0].shape)
    small = totals[..., wide_rows, :small_part].reshape(-1)
    bias_end = stats[1].size
    gain_end = bias_end + stats[2].size
    return (
        input_grad[None],
        value_rows,
        gate_rows,
        wide,
        small[:bias_end].reshape(stats[1].shape),
        small[bias_end:gain_end],
        small[gain_end:],
    )


def solution(mesh):
    placed = (
        P("dp", "sp", None),
        P("dp", "sp", None),
        P("dp", "sp", None),
        P("dp", "sp", None),
        P("dp", None),
        P("dp", None),
        P(),
        P(),
        P(),
        P(),
    )
    return jax.shard_map(
        shards,
        mesh=mesh,
        in_specs=placed,
        out_specs=(P("dp", "sp", None), P("dp", None), P("dp", None), P(), P(), P(), P()),
        check_vma=False,
    )
```
